32 devices in a mesh: ep: 8 (over z, core), tp: 4 (over y, x).
Axes of the slice: x: 2, y: 2, z: 4, core: 2. Of those that a mesh axis runs over, the one named last changes fastest.
Arguments:
- tokens: bfloat16 [1024, 2048], P('ep', 'tp'), may hold values from -6 to 6
- owner_shard: int32 [32768, 1], P('ep'), may hold values from 0 to 7; in each aligned block of 4096 rows (0 to 4095, 4096 to 8191, ...) at most 1024 rows name the same one
- local_row: int32 [32768, 1], P('ep'), may hold values from 0 to 4095
- gate_weights: float32 [1024, 32], P('ep'), may hold values from 0.05 to 1
- up_table: bfloat16 [32768, 2048], P('ep', 'tp'), may hold values from -0.125 to 0.125
- down_table: bfloat16 [32768, 2048], P('ep', 'tp'), may hold values from -6 to 6
Outputs:
- mixed: bfloat16 [1024, 2048], P('ep', 'tp')
The draws below stay inside these ranges and needn't reach their ends.
Inputs may be any that keep to these rules, and one draw needn't show every extreme that they name: `owner_shard`: within the rows of one device (128 tokens of 32 slots each, token by token) no shard is named by more than 1024 slots, a bound that some block reaches; every shard is named somewhere.
All inputs are finite; a program needn't handle non-finite values.
Results may differ from the reference program's by a relative error of at most 0.0049.
Values may be sent and summed in bfloat16 or wider, within the bound.
A program may use at most 128 MiB of HBM per device.

```python
import math
import jax
import jax.numpy as jnp
import numpy as np
from jax import lax

D = 2048
EXP_DEV = 4096
SLOTS = 32
TOK_DEV = 128
EXPERTS = 32768
TOKENS = 1024
CAP = 1024
N_EP = 8


def plant(drawn, rng, low, high):
    longest = drawn.shape.index(max(drawn.shape))
    spots = []
    for shift in (0, 1):
        where = [jax.random.randint(jax.random.fold_in(rng, axis), (), 0, length) for axis, length in enumerate(drawn.shape)]
        where[longest] = (where[longest] + shift) % drawn.shape[longest]
        spots.append(tuple(where))
    return drawn.at[spots[0]].set(low).at[spots[1]].set(high)


def block_levels(key, extent, shards, smallest, largest):
    factor_of, own = 1.0, jax.random.fold_in(key, 6)
    for axis_at, shards_of in shards:
        heights = jnp.exp(jax.random.uniform(jax.random.fold_in(own, axis_at), (shards_of,), jnp.float32, smallest / len(shards), largest / len(shards)))
        factor_of = factor_of * jnp.repeat(heights, extent[axis_at] // shards_of).reshape([-1 if axis == axis_at else 1 for axis in range(len(extent))])
    return factor_of


def rank_table(number_of, slope):
    weights = [(1 << 20) // math.isqrt(standing ** slope) + 1 for standing in range(1, number_of + 1)]
    deviation = 1 + sum(weights) // (1 << 30)
    return np.cumsum(np.array([max(1, weight // deviation) for weight in weights]))


def ranked_ids(key, extent, number_of, slope):
    table = rank_table(number_of, slope)
    pick = jax.random.randint(jax.random.fold_in(key, 1), extent, 0, int(table[number_of - 1]))
    grade = jnp.searchsorted(jnp.asarray(table, jnp.int32), pick, side="right")
    return jax.random.permutation(jax.random.fold_in(key, 2), number_of)[grade].astype(jnp.int32)


def assign_block(key, own, number, rows, number_of, top, reach, skew):
    ranking = jax.random.permutation(key, number_of)
    heavy_load, usual = shares(number_of, rows * top, reach, skew, True), shares(number_of, rows * top, reach, skew, False)
    places = jnp.arange(number_of)

    def named(lengths, turn):
        used = int((lengths > 0).sum())
        fixed = max(1, used // 4)
        moved = fixed + (places - fixed + turn * (used - fixed)) % max(1, number_of - fixed)
        return jnp.zeros((number_of,), jnp.int32).at[ranking[jnp.where(places < fixed, places, moved)]].set(jnp.asarray(lengths, jnp.int32))

    lengths = jnp.where(number % 4 == 0, named(heavy_load, number // 4), named(usual, number - number // 4 - 1))
    mixed = jax.random.permutation(jax.random.fold_in(own, 3), number_of)
    source_of, taker = mixed[0:number_of // 2 * 2:2], mixed[1:number_of // 2 * 2:2]
    room = jnp.minimum(lengths[source_of] - 1, reach - lengths[taker]) // 2
    room = jnp.where((source_of == ranking[0]) | (taker == ranking[0]) | (lengths[taker] == 0), 0, jnp.maximum(room, 0))
    moved = jax.random.randint(jax.random.fold_in(own, 4), (number_of // 2,), 0, 1 << 20) % (room + 1)
    lengths = lengths.at[source_of].add(-moved).at[taker].add(moved)
    items = jnp.searchsorted(jnp.cumsum(lengths), jnp.arange(rows * top), side="right").astype(jnp.int32)
    listing = items.reshape(top, rows).T
    listing = listing[jax.random.permutation(jax.random.fold_in(own, 1), rows)]
    turn = jax.random.randint(jax.random.fold_in(own, 2), (rows, 1), 0, top)
    return jnp.take_along_axis(listing, (jnp.arange(top)[None, :] + turn) % top, axis=1)


def shares(amount, total, limit, lean, full):
    loads = [(1 << 20) // math.isqrt(rank ** lean) + 1 for rank in range(1, amount + 1)]
    largest = limit if full else min(limit, max(-(-total // amount), total * loads[0] // sum(loads)))
    least = 1 if total - largest >= amount - 1 else 0
    holding, rest = [largest] + [least] * (amount - 1), total - largest - least * (amount - 1)
    while rest > 0:
        movable = [i for i in range(1, amount) if holding[i] < largest] or [i for i in range(1, amount) if holding[i] < limit]
        pool, left = sum([loads[i] for i in movable]), rest
        for i in movable:
            extra = min(limit - holding[i], max(1, left * loads[i] // pool), rest)
            holding[i] = holding[i] + extra
            rest = rest - extra
    return np.array(holding)


def scatter_about(key, shape, spread, most, pieces=(), dtype=jnp.bfloat16):
    factor_of = block_levels(key, shape, pieces, -0.22, 0.18) if pieces else 1.0
    result = jax.random.normal(key, shape, jnp.float32) * spread * factor_of
    return jnp.minimum(jnp.maximum(result, -most), most).astype(dtype)


def setup_inputs(seed: int = 0) -> dict:
    splits = jax.random.split(jax.random.key(seed), 7)
    tokens = scatter_about(splits[0], (TOKENS, D), 1.0, 6.0, ((0, 8), (1, 4)))
    owner_shard_keys = jax.random.split(jax.random.fold_in(splits[1], 1), (TOKENS * SLOTS) // (TOK_DEV * SLOTS))
    owner_shard_turns = jax.random.permutation(jax.random.fold_in(splits[1], 3), (TOKENS * SLOTS) // (TOK_DEV * SLOTS))
    owner_shard = jax.vmap(lambda own, number: assign_block(jax.random.fold_in(splits[1], 2), own, number, TOK_DEV * SLOTS, N_EP, 1, CAP, 2))(owner_shard_keys, owner_shard_turns).reshape((TOKENS * SLOTS, 1))
    local_row = plant(ranked_ids(splits[2], (TOKENS * SLOTS, 1), EXP_DEV, 2), jax.random.fold_in(splits[2], 3), 0, EXP_DEV - 1).astype(jnp.int32)
    gate_weights = jnp.clip(jnp.exp(math.log(1.0) - 2.9957323 * jax.random.uniform(splits[3], (TOKENS, SLOTS), jnp.float32) ** block_levels(splits[3], (TOKENS, SLOTS), ((0, 8),), -0.2, 0.2)), 0.05, 1.0)
    up_table = scatter_about(splits[4], (EXPERTS, D), D ** -0.5, 0.125, ((0, 8), (1, 4)))
    down_table = scatter_about(splits[5], (EXPERTS, D), 1.0, 6.0, ((0, 8), (1, 4)))
    return dict(tokens=tokens, owner_shard=owner_shard, local_row=local_row, gate_weights=gate_weights, up_table=up_table, down_table=down_table)


def reference(tokens, owner_shard, local_row, gate_weights, up_table, down_table):
    expert_id = (owner_shard[:, 0] * EXP_DEV + local_row[:, 0]).astype(jnp.int32)
    block_count = TOKENS // TOK_DEV
    id_blocks = expert_id.reshape(block_count, TOK_DEV, SLOTS)
    token_blocks = tokens.reshape(block_count, TOK_DEV, D)
    gate_blocks = gate_weights.reshape(block_count, TOK_DEV, SLOTS)

    def one_block(inputs):
        rows, ids, gates = inputs
        up_rows = up_table[ids].astype(jnp.float32)
        products = jnp.einsum('tsd,td->ts', up_rows, rows.astype(jnp.float32))
        slot_weight = (gates * jax.nn.gelu(products)).astype(jnp.bfloat16)
        down_rows = down_table[ids].astype(jnp.float32)
        summed = jnp.einsum('ts,tsd->td', slot_weight.astype(jnp.float32), down_rows)
        return summed.astype(jnp.bfloat16)

    mixed = lax.map(one_block, (token_blocks, id_blocks, gate_blocks))
    return mixed.reshape(TOKENS, D)
```

```python
import functools

import jax
import jax.numpy as jnp
from jax import lax
from jax.experimental import pallas as pl
from jax.experimental.pallas import tpu as pltpu
from jax.sharding import PartitionSpec as P

MESH = pl.DeviceIdType.MESH
VMEM_BYTES = 52 * 1024 * 1024


def params(number):
    return pltpu.CompilerParams(
        collective_id=number, has_side_effects=True, vmem_limit_bytes=VMEM_BYTES
    )


def vmem():
    return pl.BlockSpec(memory_space=pltpu.VMEM)


def greet(peers):
    barrier = pltpu.get_barrier_semaphore()
    for peer in peers:
        pl.semaphore_signal(barrier, inc=1, device_id=peer, device_id_type=MESH)
    pl.semaphore_wait(barrier, len(peers))


def remote(src, dst, send_sem, recv_sem, peer):
    return pltpu.make_async_remote_copy(
        src_ref=src, dst_ref=dst, send_sem=send_sem, recv_sem=recv_sem,
        device_id=peer, device_id_type=MESH,
    )


def fused_kernel(n_ep, n_tp, slots, tok_ref, aux_ref, up_hbm, down_hbm, out_ref,
                 all_tok, all_aux, up_buf, down_buf, hi_ref, lo_ref, acc_ref, pbuf, pgot, wt_ref, w_ref,
                 own, xbuf, ybuf, sbuf, rbuf,
                 local_sem, send, recv, fsend, frecv, asend, arecv, up_sem, down_sem, psend, precv,
                 xsend, xrecv, rsend, rrecv):
    chips = n_ep // 2
    me = lax.axis_index("ep")
    core = lax.rem(me, 2)
    chip = me // 2
    part = lax.axis_index("tp")
    partner = {"ep": me + 1 - 2 * core}
    experts, width = up_hbm.shape
    chunks, chunk_rows = up_buf.shape[0], up_buf.shape[1]
    tiles = experts // 128
    first = me * experts
    group, lanes = aux_ref.shape[1], aux_ref.shape[2]
    side = lanes // slots
    block = group * side
    per_tile = 128 // slots

    def at(step):
        place = chip
        for power in range(chips.bit_length() - 1):
            bit = 1 << power
            if step & bit:
                place = place + bit - 2 * bit * lax.rem(chip // bit, 2)
        return place

    def counterpart(step):
        return {"ep": at(step) * 2 + core}

    def tp_peer(step):
        return {"tp": lax.rem(part + step, n_tp)}

    up_loads = []
    for c in range(chunks):
        load = pltpu.make_async_copy(up_hbm.at[pl.ds(c * chunk_rows, chunk_rows)], up_buf.at[c], up_sem.at[c])
        load.start()
        up_loads.append(load)
    greet([partner] + [counterpart(d) for d in range(1, chips)] + [tp_peer(d) for d in range(1, n_tp)])

    pairs = ((aux_ref, all_aux), (tok_ref, all_tok))
    started = []
    local = []
    for i, (src, dst) in enumerate(pairs):
        own_copy = pltpu.make_async_copy(src, dst.at[me], local_sem.at[i])
        own_copy.start()
        local.append(own_copy)
        copy = remote(src, dst.at[me], fsend.at[i, 0], frecv.at[i, 0], partner)
        copy.start()
        started.append(copy)

    halves = group // 8
    parts = 2 * halves

    def piece(ref, number):
        rows = pl.ds(pl.multiple_of(lax.rem(number, halves) * 8, 8), 8)
        return ref.at[number // halves, rows]

    def guarded(number, action):
        if n_tp <= parts:
            action()
        else:
            pl.when(number < parts)(action)

    def aux_across(d):
        return remote(piece(aux_ref, part), piece(all_aux.at[me], part), send.at[0, d], recv.at[0, d], counterpart(d))

    def aux_around(d, t):
        slot = piece(all_aux.at[at(d) * 2 + core], part)
        return remote(slot, slot, asend.at[d, t], arecv.at[d, t], tp_peer(t))

    order = list(range(2, chips))[:1] + [1] + list(range(3, chips))
    for d in order:
        guarded(part, lambda: aux_across(d).start())
    for d in order:
        copy = remote(tok_ref, all_tok.at[me], send.at[1, d], recv.at[1, d], counterpart(d))
        copy.start()
        started.append(copy)
    down_load = pltpu.make_async_copy(down_hbm, down_buf, down_sem)
    down_load.start()

    def spread_aux(d):
        def pass_on():
            aux_across(d).wait_recv()
            for t in range(1, n_tp):
                aux_around(d, t).start()

        guarded(part, pass_on)

    def forward(d):
        source = at(d) * 2 + core
        for t in range(1, n_tp):
            guarded(lax.rem(part + n_tp - t, n_tp), lambda: aux_around(d, t).wait_recv())
        remote(tok_ref, all_tok.at[source], send.at[1, d], recv.at[1, d], partner).wait_recv()
        for i, (src, dst) in enumerate(pairs):
            copy = remote(dst.at[source], dst.at[source], fsend.at[i, d], frecv.at[i, d], partner)
            copy.start()
            started.append(copy)

    def settle_aux(d):
        def settle():
            aux_across(d).wait_send()
            for t in range(1, n_tp):
                aux_around(d, t).wait_send()

        guarded(part, settle)

    def arrive(d):
        source = at(d) * 2 + 1 - core
        for i, (src, dst) in enumerate(pairs):
            remote(src, dst.at[source], fsend.at[i, d], frecv.at[i, d], partner).wait_recv()

    lane = lax.broadcasted_iota(jnp.int32, (group, 128), 1) // slots

    def up_step(d, base):
        for b in range(2):
            for k in range(side):
                half = k // per_tile
                here = all_aux[base + b, 0, :, half * 128:(half + 1) * 128].astype(jnp.int32) - first
                fits = (here >= 0) & (here < experts) & (lane == k % per_tile)
                where = pl.ds(b * block + k, group, stride=side)
                hi_ref[where, :] = jnp.where(fits, here // 128, -1)
                lo_ref[where, :] = here & 127
        acc_ref[...] = jnp.zeros_like(acc_ref)
        if d == 0:
            for load in up_loads:
                load.wait()

        def chunk(c, carry):
            product = lax.dot_general(
                all_tok[pl.ds(base, 2)].reshape(2 * block, width), up_buf[c], (((1,), (1,)), ((), ())),
                preferred_element_type=jnp.float32,
            )
            here = chunk_rows // 128
            for r in range(0, 2 * block, 8):
                rows = slice(r, r + 8)
                acc = acc_ref[rows, :]
                hi = hi_ref[rows, :] - c * here
                lo = lo_ref[rows, :]
                for i in range(here):
                    picked = jnp.take_along_axis(
                        product[rows, i * 128:(i + 1) * 128], lo, axis=1, mode="promise_in_bounds"
                    )
                    acc = jnp.where(hi == i, picked, acc)
                acc_ref[rows, :] = acc
            return carry

        lax.fori_loop(0, chunks, chunk, 0, unroll=8)
        for b in range(2):
            for half in range(side // per_tile):
                total = None
                for k in range(half * per_tile, (half + 1) * per_tile):
                    piece = acc_ref[pl.ds(b * block + k, group, stride=side), :]
                    total = piece if total is None else total + piece
                pbuf[d, b, :, half * 128:(half + 1) * 128] = total
        copies = []
        for t in range(1, n_tp):
            copy = remote(pbuf.at[d], pgot.at[d, t], psend.at[d, t], precv.at[d, t], tp_peer(t))
            copy.start()
            copies.append(copy)
        started.extend(copies)
        return copies

    def row_keys(count):
        keys = lax.broadcasted_iota(jnp.int32, (count, lanes), 0).astype(jnp.float32)
        return keys.astype(jnp.bfloat16).reshape(count // 16, 16, lanes)

    row_key = row_keys(tiles * side)
    low_key = row_keys(128)
    turn = lax.broadcasted_iota(jnp.int32, (16, lanes), 1) // slots
    zero = jnp.zeros((1, 16, lanes), jnp.bfloat16)
    one = jnp.ones((1, 16, lanes), jnp.bfloat16)

    def narrow(x):
        return x.astype(jnp.float32).astype(jnp.bfloat16)[None]

    pending = []
    returned = []
    places = []

    def down_step(d, base, copies):
        total = pbuf[d]
        for t, copy in enumerate(copies):
            copy.wait_recv()
            total += pgot[d, t + 1]
        gate = all_aux[pl.ds(base, 2), 1]
        wt_ref[...] = (gate * jax.nn.gelu(total)).astype(jnp.bfloat16).astype(jnp.float32)

        def spread(b, j):
            here = jnp.broadcast_to(all_aux[base + b, 0, pl.ds(j, 1), :], (16, lanes)).astype(jnp.int32) - first
            weight = jnp.broadcast_to(wt_ref[b, pl.ds(j, 1), :], (16, lanes)).astype(jnp.bfloat16)[None]
            fits = (here >= 0) & (here < experts)
            key = narrow(jnp.where(fits, (here // 128) * side + turn, -1))
            left = jnp.where(row_key == key, weight, zero).reshape(tiles * side, lanes)
            right = jnp.where(low_key == narrow(here & 127), one, zero).reshape(128, lanes)
            wide = lax.dot_general(left, right, (((1,), (1,)), ((), ())), preferred_element_type=jnp.float32)
            return wide.reshape(tiles, side, 128)

        def build(x, carry):
            b = x // (group // 2)
            j = lax.rem(x, group // 2) * 2
            both = jnp.concatenate([spread(b, j), spread(b, j + 1)], axis=1).astype(jnp.bfloat16)
            for h in range(tiles):
                w_ref[pl.ds(pl.multiple_of(x * 2 * side, 2 * side), 2 * side), h * 128:(h + 1) * 128] = both[h]
            return carry

        lax.fori_loop(0, group, build, 0, unroll=8)
        if pending:
            finish(*pending.pop())
        if d == 0:
            down_load.wait()
        sums = jnp.dot(w_ref[...], down_buf[...], preferred_element_type=jnp.float32)
        low, high = sums[:block], sums[block:]
        own[d] = jnp.where(core == 0, low, high)
        xbuf[d] = jnp.where(core == 0, high, low).astype(jnp.bfloat16)
        copy = remote(xbuf.at[d], ybuf.at[d], xsend.at[d], xrecv.at[d], partner)
        copy.start()
        started.append(copy)
        return copy

    def finish(d, copy):
        copy.wait_recv()
        if d == 0:
            return
        sbuf[d] = (own[d] + ybuf[d].astype(jnp.float32)).astype(jnp.bfloat16)
        copy = remote(sbuf.at[d], rbuf.at[d], rsend.at[d], rrecv.at[d], counterpart(d))
        copy.start()
        returned.append(copy)
        places.append(d)

    def base_of(d):
        return at(d) * 2 if d else chip * 2

    for copy in local:
        copy.wait()
    sending = {}

    def up(d):
        arrive(d)
        sending[d] = up_step(d, base_of(d))

    def down(d):
        pending.append((d, down_step(d, base_of(d), sending[d])))

    up(0)
    for d in order:
        spread_aux(d)
    down(0)
    early, late = order[:2], order[2:]
    for d in early:
        forward(d)
        up(d)
    for d in late:
        forward(d)
    down(early[0])
    for d in late:
        up(d)
    down(early[1])
    for d in late:
        down(d)
    finish(*pending.pop())
    total = own[0] + ybuf[0].astype(jnp.float32)
    for d, copy in enumerate(returned):
        copy.wait_recv()
        total += rbuf[places[d]].astype(jnp.float32)
    out_ref[...] = total.astype(jnp.bfloat16)
    for d in range(1, chips):
        settle_aux(d)
    for copy in started + returned:
        copy.wait_send()


def on_device(tokens, owner_shard, local_row, gate_weights, up_table, down_table):
    n_ep, n_tp = lax.axis_size("ep"), lax.axis_size("tp")
    count, width = tokens.shape
    slots = gate_weights.shape[1]
    experts = up_table.shape[0]
    side = 8
    group, lanes = count // side, side * slots
    chips = n_ep // 2
    ids = owner_shard[:, 0] * experts + local_row[:, 0]
    aux = jnp.stack([ids.astype(jnp.float32).reshape(group, lanes), gate_weights.reshape(group, lanes)])
    dma = pltpu.SemaphoreType.DMA
    chunks = experts // 512
    wide = (chips, count, width)
    anywhere = pl.BlockSpec(memory_space=pl.ANY)
    return pl.pallas_call(
        functools.partial(fused_kernel, n_ep, n_tp, slots),
        out_shape=jax.ShapeDtypeStruct((count, width), jnp.bfloat16),
        in_specs=[vmem(), vmem(), anywhere, anywhere],
        out_specs=vmem(),
        scratch_shapes=[
            pltpu.VMEM((n_ep, count, width), jnp.bfloat16),
            pltpu.VMEM((n_ep, 2, group, lanes), jnp.float32),
            pltpu.VMEM((chunks, experts // chunks, width), jnp.bfloat16),
            pltpu.VMEM((experts, width), jnp.bfloat16),
            pltpu.VMEM((2 * count, 128), jnp.int32),
            pltpu.VMEM((2 * count, 128), jnp.int32),
            pltpu.VMEM((2 * count, 128), jnp.float32),
            pltpu.VMEM((chips, 2, group, lanes), jnp.float32),
            pltpu.VMEM((chips, n_tp, 2, group, lanes), jnp.float32),
            pltpu.VMEM((2, group, lanes), jnp.float32),
            pltpu.VMEM((2 * count, experts), jnp.bfloat16),
            pltpu.VMEM(wide, jnp.float32),
            pltpu.VMEM(wide, jnp.bfloat16),
            pltpu.VMEM(wide, jnp.bfloat16),
            pltpu.VMEM(wide, jnp.bfloat16),
            pltpu.VMEM(wide, jnp.bfloat16),
            dma((2,)), dma((2, chips)), dma((2, chips)), dma((2, chips)), dma((2, chips)), dma((chips, n_tp)), dma((chips, n_tp)),
            dma((chunks,)), dma, dma((chips, n_tp)), dma((chips, n_tp)),
            dma((chips,)), dma((chips,)), dma((chips,)), dma((chips,)),
        ],
        compiler_params=params(0),
        name="retrieve",
    )(tokens, aux, up_table, down_table)


def solution(mesh):
    return jax.shard_map(
        on_device,
        mesh=mesh,
        in_specs=(
            P("ep", "tp"),
            P("ep", None),
            P("ep", None),
            P("ep", None),
            P("ep", "tp"),
            P("ep", "tp"),
        ),
        out_specs=P("ep", "tp"),
        check_vma=False,
    )
```

```python
import functools

import jax
import jax.numpy as jnp
from jax import lax
from jax.experimental import pallas as pl
from jax.experimental.pallas import tpu as pltpu
from jax.sharding import PartitionSpec as P

MESH = pl.DeviceIdType.MESH
VMEM_BYTES = 52 * 1024 * 1024


def params(number):
    return pltpu.CompilerParams(
        collective_id=number, has_side_effects=True, vmem_limit_bytes=VMEM_BYTES
    )


def vmem():
    return pl.BlockSpec(memory_space=pltpu.VMEM)


def greet(peers):
    barrier = pltpu.get_barrier_semaphore()
    for peer in peers:
        pl.semaphore_signal(barrier, inc=1, device_id=peer, device_id_type=MESH)
    pl.semaphore_wait(barrier, len(peers))


def remote(src, dst, send_sem, recv_sem, peer):
    return pltpu.make_async_remote_copy(
        src_ref=src, dst_ref=dst, send_sem=send_sem, recv_sem=recv_sem,
        device_id=peer, device_id_type=MESH,
    )


def fused_kernel(n_ep, n_tp, slots, tok_ref, ids_ref, gate_ref, up_hbm, down_hbm, out_ref,
                 aux_ref, turned_ref, all_tok, all_aux, up_buf, down_buf, hi_ref, lo_ref, acc_ref, pbuf, pgot, wt_ref, w_ref,
                 own, xbuf, ybuf, sbuf, rbuf,
                 local_sem, send, recv, fsend, frecv, asend, arecv, up_sem, down_sem, psend, precv,
                 xsend, xrecv, rsend, rrecv):
    chips = n_ep // 2
    me = lax.axis_index("ep")
    core = lax.rem(me, 2)
    chip = me // 2
    part = lax.axis_index("tp")
    partner = {"ep": me + 1 - 2 * core}
    experts, width = up_hbm.shape
    chunks, chunk_rows = up_buf.shape[0], up_buf.shape[1]
    tiles = experts // 128
    first = me * experts
    group, lanes = aux_ref.shape[1], aux_ref.shape[2]
    side = lanes // slots
    block = group * side
    per_tile = 128 // slots

    def at(step):
        place = chip
        for power in range(chips.bit_length() - 1):
            bit = 1 << power
            if step & bit:
                place = place + bit - 2 * bit * lax.rem(chip // bit, 2)
        return place

    def counterpart(step):
        return {"ep": at(step) * 2 + core}

    def tp_peer(step):
        return {"tp": lax.rem(part + step, n_tp)}

    up_loads = []
    for c in range(chunks):
        load = pltpu.make_async_copy(up_hbm.at[pl.ds(c * chunk_rows, chunk_rows)], up_buf.at[c], up_sem.at[c])
        load.start()
        up_loads.append(load)
    turned_ref[...] = jnp.concatenate([gate_ref[...]] * per_tile, axis=0).T
    place = lax.broadcasted_iota(jnp.int32, (group, 128), 1) // slots
    for half in range(side // per_tile):
        columns = slice(half * 128, (half + 1) * 128)
        aux_ref[0, :, columns] = ids_ref[pl.ds(half, group, stride=lanes // 128), :]
        gates = turned_ref[pl.ds(half * per_tile, group, stride=side), :]
        for k in range(1, per_tile):
            rows = pl.ds(half * per_tile + k, group, stride=side)
            gates = jnp.where(place == k, turned_ref[rows, :], gates)
        aux_ref[1, :, columns] = gates
    greet([partner] + [counterpart(d) for d in range(1, chips)] + [tp_peer(d) for d in range(1, n_tp)])

    pairs = ((aux_ref, all_aux), (tok_ref, all_tok))
    started = []
    local = []
    for i, (src, dst) in enumerate(pairs):
        own_copy = pltpu.make_async_copy(src, dst.at[me], local_sem.at[i])
        own_copy.start()
        local.append(own_copy)
        copy = remote(src, dst.at[me], fsend.at[i, 0], frecv.at[i, 0], partner)
        copy.start()
        started.append(copy)

    halves = group // 8
    parts = 2 * halves

    def piece(ref, number):
        rows = pl.ds(pl.multiple_of(lax.rem(number, halves) * 8, 8), 8)
        return ref.at[number // halves, rows]

    def guarded(number, action):
        if n_tp <= parts:
            action()
        else:
            pl.when(number < parts)(action)

    def aux_across(d):
        return remote(piece(aux_ref, part), piece(all_aux.at[me], part), send.at[0, d], recv.at[0, d], counterpart(d))

    def aux_around(d, t):
        slot = piece(all_aux.at[at(d) * 2 + core], part)
        return remote(slot, slot, asend.at[d, t], arecv.at[d, t], tp_peer(t))

    def aux_whole():
        return remote(aux_ref, all_aux.at[me], send.at[0, 1], recv.at[0, 1], counterpart(1))

    aux_whole().start()
    for d in range(2, chips):
        guarded(part, lambda: aux_across(d).start())
    def send_tokens(d):
        copy = remote(tok_ref, all_tok.at[me], send.at[1, d], recv.at[1, d], counterpart(d))
        copy.start()
        started.append(copy)

    send_tokens(1)
    down_load = pltpu.make_async_copy(down_hbm, down_buf, down_sem)
    down_load.start()

    def spread_aux(d):
        def pass_on():
            aux_across(d).wait_recv()
            for t in range(1, n_tp):
                aux_around(d, t).start()

        guarded(part, pass_on)

    def forward(d):
        source = at(d) * 2 + core
        if d == 1:
            aux_whole().wait_recv()
        for t in range(1, n_tp if d > 1 else 1):
            guarded(lax.rem(part + n_tp - t, n_tp), lambda: aux_around(d, t).wait_recv())
        remote(tok_ref, all_tok.at[source], send.at[1, d], recv.at[1, d], partner).wait_recv()
        for i, (src, dst) in enumerate(pairs):
            copy = remote(dst.at[source], dst.at[source], fsend.at[i, d], frecv.at[i, d], partner)
            copy.start()
            started.append(copy)

    def settle_aux(d):
        def settle():
            aux_across(d).wait_send()
            for t in range(1, n_tp):
                aux_around(d, t).wait_send()

        guarded(part, settle)

    def arrive(d):
        source = at(d) * 2 + 1 - core
        for i, (src, dst) in enumerate(pairs):
            remote(src, dst.at[source], fsend.at[i, d], frecv.at[i, d], partner).wait_recv()

    lane = lax.broadcasted_iota(jnp.int32, (group, 128), 1) // slots

    def up_step(d, base):
        for b in range(2):
            for k in range(side):
                half = k // per_tile
                here = all_aux[base + b, 0, :, half * 128:(half + 1) * 128].astype(jnp.int32) - first
                fits = (here >= 0) & (here < experts) & (lane == k % per_tile)
                where = pl.ds(b * block + k, group, stride=side)
                hi_ref[where, :] = jnp.where(fits, here // 128, -1)
                lo_ref[where, :] = here & 127
        acc_ref[...] = jnp.zeros_like(acc_ref)
        if d == 0:
            for load in up_loads:
                load.wait()

        def chunk(c, carry):
            product = lax.dot_general(
                all_tok[pl.ds(base, 2)].reshape(2 * block, width), up_buf[c], (((1,), (1,)), ((), ())),
                preferred_element_type=jnp.float32,
            )
            here = chunk_rows // 128
            for r in range(0, 2 * block, 8):
                rows = slice(r, r + 8)
                acc = acc_ref[rows, :]
                hi = hi_ref[rows, :] - c * here
                lo = lo_ref[rows, :]
                for i in range(here):
                    picked = jnp.take_along_axis(
                        product[rows, i * 128:(i + 1) * 128], lo, axis=1, mode="promise_in_bounds"
                    )
                    acc = jnp.where(hi == i, picked, acc)
                acc_ref[rows, :] = acc
            return carry

        lax.fori_loop(0, chunks, chunk, 0, unroll=8)
        for b in range(2):
            for half in range(side // per_tile):
                total = None
                for k in range(half * per_tile, (half + 1) * per_tile):
                    piece = acc_ref[pl.ds(b * block + k, group, stride=side), :]
                    total = piece if total is None else total + piece
                pbuf[d, b, :, half * 128:(half + 1) * 128] = total
        copies = []
        if pending:
            finish(*pending.pop())
        for t in range(1, n_tp):
            copy = remote(pbuf.at[d], pgot.at[d, t], psend.at[d, t], precv.at[d, t], tp_peer(t))
            copy.start()
            copies.append(copy)
        started.extend(copies)
        return copies

    def row_keys(count):
        keys = lax.broadcasted_iota(jnp.int32, (count, lanes), 0).astype(jnp.float32)
        return keys.astype(jnp.bfloat16).reshape(count // 16, 16, lanes)

    row_key = row_keys(tiles * side)
    low_key = row_keys(128)
    turn = lax.broadcasted_iota(jnp.int32, (16, lanes), 1) // slots
    zero = jnp.zeros((1, 16, lanes), jnp.bfloat16)
    one = jnp.ones((1, 16, lanes), jnp.bfloat16)

    def narrow(x):
        return x.astype(jnp.float32).astype(jnp.bfloat16)[None]

    pending = []
    returned = []
    places = []

    def down_step(d, base, copies):
        total = pbuf[d]
        for t, copy in enumerate(copies):
            copy.wait_recv()
            total += pgot[d, t + 1]
        gate = all_aux[pl.ds(base, 2), 1]
        wt_ref[...] = (gate * jax.nn.gelu(total)).astype(jnp.bfloat16).astype(jnp.float32)

        def spread(b, j):
            here = jnp.broadcast_to(all_aux[base + b, 0, pl.ds(j, 1), :], (16, lanes)).astype(jnp.int32) - first
            weight = jnp.broadcast_to(wt_ref[b, pl.ds(j, 1), :], (16, lanes)).astype(jnp.bfloat16)[None]
            fits = (here >= 0) & (here < experts)
            key = narrow(jnp.where(fits, (here // 128) * side + turn, -1))
            left = jnp.where(row_key == key, weight, zero).reshape(tiles * side, lanes)
            right = jnp.where(low_key == narrow(here & 127), one, zero).reshape(128, lanes)
            wide = lax.dot_general(left, right, (((1,), (1,)), ((), ())), preferred_element_type=jnp.float32)
            return wide.reshape(tiles, side, 128)

        def build(x, carry):
            b = x // (group // 2)
            j = lax.rem(x, group // 2) * 2
            both = jnp.concatenate([spread(b, j), spread(b, j + 1)], axis=1).astype(jnp.bfloat16)
            for h in range(tiles):
                w_ref[pl.ds(pl.multiple_of(x * 2 * side, 2 * side), 2 * side), h * 128:(h + 1) * 128] = both[h]
            return carry

        lax.fori_loop(0, group, build, 0, unroll=8)
        if pending:
            finish(*pending.pop())
        if d == 0:
            down_load.wait()
        sums = jnp.dot(w_ref[...], down_buf[...], preferred_element_type=jnp.float32)
        low, high = sums[:block], sums[block:]
        own[d] = jnp.where(core == 0, low, high)
        xbuf[d] = jnp.where(core == 0, high, low).astype(jnp.bfloat16)
        copy = remote(xbuf.at[d], ybuf.at[d], xsend.at[d], xrecv.at[d], partner)
        copy.start()
        started.append(copy)
        return copy

    def finish(d, copy):
        copy.wait_recv()
        if d == 0:
            return
        sbuf[d] = (own[d] + ybuf[d].astype(jnp.float32)).astype(jnp.bfloat16)
        copy = remote(sbuf.at[d], rbuf.at[d], rsend.at[d], rrecv.at[d], counterpart(d))
        copy.start()
        returned.append(copy)
        places.append(d)

    def base_of(d):
        return at(d) * 2 if d else chip * 2

    for copy in local:
        copy.wait()
    sending = {}

    def up(d):
        if d:
            arrive(d)
        sending[d] = up_step(d, base_of(d))

    def down(d):
        pending.append((d, down_step(d, base_of(d), sending[d])))

    arrive(0)
    last = chips - 1
    send_tokens(2)
    up(0)
    for d in range(3, chips):
        send_tokens(d)
    forward(1)
    for d in range(2, chips):
        spread_aux(d)
    up(1)
    forward(2)
    up(2)
    forward(3)
    down(0)
    for d in range(2, last):
        down(d)
        up(d + 1)
        if d + 2 < chips:
            forward(d + 2)
    down(1)
    down(last)
    finish(*pending.pop())
    total = own[0] + ybuf[0].astype(jnp.float32)
    for d, copy in enumerate(returned):
        copy.wait_recv()
        total += rbuf[places[d]].astype(jnp.float32)
    out_ref[...] = total.astype(jnp.bfloat16)
    aux_whole().wait_send()
    for d in range(2, chips):
        settle_aux(d)
    for copy in started + returned:
        copy.wait_send()


def on_device(tokens, owner_shard, local_row, gate_weights, up_table, down_table):
    n_ep, n_tp = lax.axis_size("ep"), lax.axis_size("tp")
    count, width = tokens.shape
    slots = gate_weights.shape[1]
    experts = up_table.shape[0]
    side = 8
    group, lanes = count // side, side * slots
    chips = n_ep // 2
    dense = (count * slots // 128, 128)
    ids = (owner_shard[:, 0] * experts + local_row[:, 0]).astype(jnp.float32)
    dma = pltpu.SemaphoreType.DMA
    chunks = experts // 512
    wide = (chips, count, width)
    anywhere = pl.BlockSpec(memory_space=pl.ANY)
    return pl.pallas_call(
        functools.partial(fused_kernel, n_ep, n_tp, slots),
        out_shape=jax.ShapeDtypeStruct((count, width), jnp.bfloat16),
        in_specs=[vmem(), vmem(), vmem(), anywhere, anywhere],
        out_specs=vmem(),
        scratch_shapes=[
            pltpu.VMEM((2, group, lanes), jnp.float32),
            pltpu.VMEM((count, 128), jnp.float32),
            pltpu.VMEM((n_ep, count, width), jnp.bfloat16),
            pltpu.VMEM((n_ep, 2, group, lanes), jnp.float32),
            pltpu.VMEM((chunks, experts // chunks, width), jnp.bfloat16),
            pltpu.VMEM((experts, width), jnp.bfloat16),
            pltpu.VMEM((2 * count, 128), jnp.int32),
            pltpu.VMEM((2 * count, 128), jnp.int32),
            pltpu.VMEM((2 * count, 128), jnp.float32),
            pltpu.VMEM((chips, 2, group, lanes), jnp.float32),
            pltpu.VMEM((chips, n_tp, 2, group, lanes), jnp.float32),
            pltpu.VMEM((2, group, lanes), jnp.float32),
            pltpu.VMEM((2 * count, experts), jnp.bfloat16),
            pltpu.VMEM(wide, jnp.float32),
            pltpu.VMEM(wide, jnp.bfloat16),
            pltpu.VMEM(wide, jnp.bfloat16),
            pltpu.VMEM(wide, jnp.bfloat16),
            pltpu.VMEM(wide, jnp.bfloat16),
            dma((2,)), dma((2, chips)), dma((2, chips)), dma((2, chips)), dma((2, chips)), dma((chips, n_tp)), dma((chips, n_tp)),
            dma((chunks,)), dma, dma((chips, n_tp)), dma((chips, n_tp)),
            dma((chips,)), dma((chips,)), dma((chips,)), dma((chips,)),
        ],
        compiler_params=params(0),
        name="retrieve",
    )(tokens, ids.reshape(dense), gate_weights.T, up_table, down_table)


def solution(mesh):
    return jax.shard_map(
        on_device,
        mesh=mesh,
        in_specs=(
            P("ep", "tp"),
            P("ep", None),
            P("ep", None),
            P("ep", None),
            P("ep", "tp"),
            P("ep", "tp"),
        ),
        out_specs=P("ep", "tp"),
        check_vma=False,
    )
```
